32 devices in a mesh: ep: 8 (over z, x), tp: 4 (over y, core).
Axes of the slice: x: 2, y: 2, z: 4, core: 2. Of those that a mesh axis runs over, the one named last changes fastest.
Arguments:
- conv_value: bfloat16 [8192, 1024], P('ep', 'tp'), may hold values from -600 to 600
- conv_gate: bfloat16 [8192, 1024], P('ep', 'tp'), may hold values from -8 to 8
- depth_weight: float32 [31, 1024], replicated, may hold values from -1 to 1
- norm_gain: float32 [1024], replicated, may hold values from 0.1 to 1.9
- norm_shift: float32 [1024], replicated, may hold values from -3 to 3
- conv_out_weight: bfloat16 [1024, 2048], P('tp'), may hold values from -0.1875 to 0.1875
- moe_input: bfloat16 [12288, 2048], P(('ep', 'tp')), may hold values from -6 to 6
- moe_gain: float32 [2048], replicated, may hold values from 0.1 to 1.9
- route_experts: int32 [12288, 2], P(('ep', 'tp')), may hold values from 0 to 7, as said below
- route_scores: float32 [12288, 2], P(('ep', 'tp')), may hold values from -8 to 8
- expert_gate: bfloat16 [8, 2048, 512], P('ep'), may hold values from -0.125 to 0.125
- expert_up: bfloat16 [8, 2048, 512], P('ep'), may hold values from -0.125 to 0.125
- expert_down: bfloat16 [8, 512, 2048], P('ep'), may hold values from -1 to 1
Outputs:
- conv_out: bfloat16 [8192, 2048], P(('ep', 'tp'))
- moe_out: bfloat16 [12288, 2048], P(('ep', 'tp'))
The draws below stay inside these ranges and needn't reach their ends.
Inputs may be any that keep to these rules, and one draw needn't show every extreme that they name: `route_experts`: each row names two different experts that lie in one group of 2 consecutive experts.
All inputs are finite; a program needn't handle non-finite values.
Results may differ from the reference program's by a relative error of at most 0.009.
Values may be sent and summed in bfloat16 or wider, within the bound.
A program may use at most 128 MiB of HBM per device.

```python
import jax
import jax.numpy as jnp
from jax import lax

D = 2048
CONV = 1024
FF = 512
KERNEL = 31
GROUPS = 4
TOP = 2
TOK_B = 384
EXPERTS = 8
GROUP_EXP = 2
CAP = 144
TOKENS_A = 8192
TOKENS_B = 12288
N_EP = 8
N_TP = 4


def draw_conv_value(key, part):
    keys = jax.random.split(jax.random.fold_in(key, 31), 2)
    column_scale = 10.0 ** (jnp.arange(CONV, dtype=jnp.float32) / CONV)
    base = jnp.clip(jax.random.normal(keys[0], (TOKENS_A, CONV), jnp.float32), -4.0, 4.0)
    row_scale = 10.0 ** jax.random.uniform(keys[1], (TOKENS_A, 1), jnp.float32)
    return (base * row_scale * column_scale[None, :]).astype(jnp.bfloat16)


def group_order(key):
    return jax.random.permutation(key, GROUP_EXP)


def draw_route_experts(key, part):
    keys = jax.random.split(jax.random.fold_in(key, 17), 7)
    order_groups = jax.random.permutation(keys[0], GROUPS)
    group_pick = jnp.minimum(jax.random.randint(keys[1], (TOKENS_B,), 0, GROUPS), jax.random.randint(keys[2], (TOKENS_B,), 0, GROUPS))
    group_id = order_groups[group_pick]
    orders = jax.vmap(group_order)(jax.random.split(keys[3], GROUPS))
    first_pick = jnp.minimum(jax.random.randint(keys[4], (TOKENS_B,), 0, GROUP_EXP), jax.random.randint(keys[5], (TOKENS_B,), 0, GROUP_EXP))
    second_pick = (first_pick + 1 + jax.random.randint(keys[6], (TOKENS_B,), 0, GROUP_EXP - 1)) % GROUP_EXP
    first = group_id * GROUP_EXP + orders[group_id, first_pick]
    second = group_id * GROUP_EXP + orders[group_id, second_pick]
    return jnp.stack([first, second], axis=1).astype(jnp.int32)


def shard_levels(rng, dims, shards, smallest, top_value):
    def one(position, shards_of):
        steps = jax.random.uniform(jax.random.fold_in(jax.random.fold_in(rng, 6), position), (shards_of,), jnp.float32, smallest / len(shards), top_value / len(shards))
        return jnp.repeat(jnp.exp(steps), dims[position] // shards_of).reshape((-1,) + (1,) * (len(dims) - position - 1))

    gain = one(*shards[0])
    for cut in shards[1:]:
        gain = gain * one(*cut)
    return gain


def normal_values(key, dims, deviation, reach, cuts=(), kind=jnp.bfloat16):
    result = jax.random.normal(key, dims, jnp.float32) * deviation
    if len(cuts) > 0:
        result = shard_levels(key, dims, cuts, -0.22, 0.18) * result
    return jnp.clip(result, min=-reach, max=reach).astype(kind)


def setup_inputs(seed: int = 0) -> dict:
    arg_keys = jax.random.split(jax.random.key(seed), 14)
    conv_value = draw_conv_value(jax.random.fold_in(arg_keys[13], 71), 0)
    conv_gate = normal_values(arg_keys[1], (TOKENS_A, CONV), 1.5, 8.0, ((0, 8), (1, 4)))
    depth_weight = normal_values(arg_keys[2], (KERNEL, CONV), KERNEL ** -0.5, 1.0, (), jnp.float32)
    norm_gain = jnp.clip(1.0 + 0.18 * jax.random.normal(arg_keys[3], (CONV,), jnp.float32), 0.1, 1.9)
    norm_shift = normal_values(arg_keys[4], (CONV,), 0.5, 3.0, (), jnp.float32)
    conv_out_weight = normal_values(arg_keys[5], (CONV, D), CONV ** -0.5, 0.1875, ((0, 4),))
    moe_input = normal_values(arg_keys[6], (TOKENS_B, D), 1.0, 6.0, ((0, 32),))
    moe_gain = jnp.clip(1.0 + 0.18 * jax.random.normal(arg_keys[7], (D,), jnp.float32), 0.1, 1.9)
    route_experts = draw_route_experts(jax.random.fold_in(arg_keys[13], 71), 0)
    route_scores = normal_values(arg_keys[9], (TOKENS_B, TOP), 1.5, 8.0, ((0, 32),), jnp.float32)
    expert_gate = normal_values(arg_keys[10], (EXPERTS, D, FF), D ** -0.5, 0.125, ((0, 8),))
    expert_up = normal_values(arg_keys[11], (EXPERTS, D, FF), D ** -0.5, 0.125, ((0, 8),))
    expert_down = normal_values(arg_keys[12], (EXPERTS, FF, D), (FF // 16) ** -0.5, 1.0, ((0, 8),))
    return dict(conv_value=conv_value, conv_gate=conv_gate, depth_weight=depth_weight, norm_gain=norm_gain, norm_shift=norm_shift, conv_out_weight=conv_out_weight, moe_input=moe_input, moe_gain=moe_gain, route_experts=route_experts, route_scores=route_scores, expert_gate=expert_gate, expert_up=expert_up, expert_down=expert_down)


def conv_part(conv_value, conv_gate, depth_weight, norm_gain, norm_shift, conv_out_weight):
    gated = (conv_value.astype(jnp.float32) * jax.nn.sigmoid(conv_gate.astype(jnp.float32))).astype(jnp.bfloat16)
    padded = jnp.concatenate([jnp.zeros((KERNEL - 1, CONV), jnp.bfloat16), gated], 0).astype(jnp.float32)
    filtered = jnp.zeros((TOKENS_A, CONV), jnp.float32)
    for offset in range(KERNEL):
        filtered = filtered + depth_weight[offset] * padded[offset:offset + TOKENS_A]
    center = lax.optimization_barrier(jnp.mean(filtered, axis=-1, keepdims=True))
    spread = lax.optimization_barrier(jnp.mean(filtered * filtered, axis=-1, keepdims=True)) - center * center
    normed = (filtered - center) * lax.rsqrt(spread + 1e-05) * norm_gain + norm_shift
    activated = jax.nn.silu(normed).astype(jnp.bfloat16)
    block_width = CONV // N_TP
    summed = jnp.zeros((TOKENS_A, D), jnp.float32)
    for column_block in range(N_TP):
        low = column_block * block_width
        partial_value = jnp.dot(activated[:, low:low + block_width], conv_out_weight[low:low + block_width], preferred_element_type=jnp.float32).astype(jnp.bfloat16)
        summed = summed + partial_value.astype(jnp.float32)
    return summed.astype(jnp.bfloat16)

def moe_part(moe_input, moe_gain, route_experts, route_scores, expert_gate, expert_up, expert_down):
    widened = moe_input.astype(jnp.float32)
    normal_in = (widened * lax.rsqrt(lax.optimization_barrier(jnp.mean(widened * widened, axis=-1, keepdims=True)) + 1e-06) * moe_gain).astype(jnp.bfloat16)
    sources = N_EP * N_TP
    chosen = route_experts.reshape(sources, TOK_B * TOP)
    onehot = (chosen[:, :, None] == jnp.arange(EXPERTS, dtype=jnp.int32)[None, None, :]).astype(jnp.int32)
    slot_rank = lax.optimization_barrier(jnp.sum(jnp.cumsum(onehot, axis=1) * onehot, axis=-1)) - 1
    within_cap = slot_rank < CAP
    source_ids = jnp.arange(sources, dtype=jnp.int32)[:, None]
    token_index = source_ids * TOK_B + jnp.arange(TOK_B * TOP, dtype=jnp.int32)[None, :] // TOP
    per_expert = sources * CAP
    slot_index = jnp.where(within_cap, chosen * per_expert + source_ids * CAP + slot_rank, EXPERTS * per_expert).astype(jnp.int32)
    slot_token = jnp.full((EXPERTS * per_expert,), TOKENS_B, jnp.int32).at[slot_index.reshape(-1)].set(token_index.reshape(-1), mode='drop')
    group_gate = jax.nn.sigmoid(route_scores[:, 0])
    weights = jnp.stack([group_gate * jax.nn.sigmoid(route_scores[:, 1]), group_gate * jax.nn.sigmoid(-route_scores[:, 1])], axis=-1)
    slot_weight = jnp.zeros((EXPERTS * per_expert,), jnp.float32).at[slot_index.reshape(-1)].set(weights.reshape(-1), mode='drop')
    padded_in = jnp.concatenate([normal_in, jnp.zeros((1, D), jnp.bfloat16)], 0)

    def apply_expert(summed, inputs):
        gate_matrix, up_matrix, down_matrix, tokens_here, weight_here = inputs
        picked_rows = padded_in[tokens_here]
        gate_act = jnp.dot(picked_rows, gate_matrix, preferred_element_type=jnp.float32)
        up_act = jnp.dot(picked_rows, up_matrix, preferred_element_type=jnp.float32)
        inner = (jax.nn.silu(gate_act) * up_act).astype(jnp.bfloat16)
        expert_rows = jnp.dot(inner, down_matrix, preferred_element_type=jnp.float32).astype(jnp.bfloat16)
        summed = summed.at[tokens_here].add(weight_here[:, None] * expert_rows.astype(jnp.float32), mode='drop')
        return (summed, None)
    summed, _ = lax.scan(apply_expert, jnp.zeros((TOKENS_B, D), jnp.float32), (expert_gate, expert_up, expert_down, slot_token.reshape(EXPERTS, per_expert), slot_weight.reshape(EXPERTS, per_expert)))
    return summed.astype(jnp.bfloat16)

def reference(conv_value, conv_gate, depth_weight, norm_gain, norm_shift, conv_out_weight, moe_input, moe_gain, route_experts, route_scores, expert_gate, expert_up, expert_down):
    conv_out = conv_part(conv_value, conv_gate, depth_weight, norm_gain, norm_shift, conv_out_weight)
    moe_out = moe_part(moe_input, moe_gain, route_experts, route_scores, expert_gate, expert_up, expert_down)
    return (conv_out, moe_out)
```

```python
import jax
import jax.numpy as jnp
from jax import lax
from jax.sharding import PartitionSpec as P

GROUPS = 4
TOP = 2


def passed_along(x, axis, by):
    peers = lax.axis_size(axis)
    pairs = [(i, i + by) for i in range(peers) if 0 <= i + by < peers]
    return lax.ppermute(x, axis, pairs)


def gate_and_halo(conv_value, conv_gate, reach):
    gated = (conv_value.astype(jnp.float32) * jax.nn.sigmoid(conv_gate.astype(jnp.float32))).astype(
        jnp.bfloat16
    )
    return gated, passed_along(gated[gated.shape[0] - reach :], "ep", 1)


def conv_half(conv_value, gated, earlier, depth_weight, norm_gain, norm_shift, conv_out_weight):
    channels = conv_value.shape[1]
    length = conv_value.shape[0]
    first_col = lax.axis_index("tp") * channels
    taps = lax.dynamic_slice_in_dim(depth_weight, first_col, channels, 1)
    gains = lax.dynamic_slice_in_dim(norm_gain, first_col, channels, 0)
    shifts = lax.dynamic_slice_in_dim(norm_shift, first_col, channels, 0)
    reach = taps.shape[0] - 1
    padded = jnp.concatenate([earlier, gated], 0).astype(jnp.float32)
    filtered = taps[0] * padded[0:length]
    for offset in range(1, reach + 1):
        filtered = filtered + taps[offset] * padded[offset : offset + length]
    sums, squares = lax.psum(
        (jnp.sum(filtered, axis=1), jnp.sum(filtered * filtered, axis=1)), "tp"
    )
    all_channels = channels * lax.axis_size("tp")
    center = (sums / all_channels)[:, None]
    spread = (squares / all_channels)[:, None] - center * center
    normed = (filtered - center) * lax.rsqrt(spread + 1e-05) * gains + shifts
    activated = jax.nn.silu(normed).astype(jnp.bfloat16)
    partial_value = jnp.dot(activated, conv_out_weight, preferred_element_type=jnp.float32)
    return lax.psum_scatter(
        partial_value.astype(jnp.bfloat16).astype(jnp.float32).astype(jnp.bfloat16),
        "tp",
        scatter_dimension=0,
        tiled=True,
    )


def moe_half(moe_input, moe_gain, route_experts, route_scores, expert_gate, expert_up, expert_down):
    rows = moe_input.shape[0]
    model_width = moe_input.shape[1]
    experts_all = lax.axis_size("ep")
    capacity = 2 * (3 * TOP * rows // (4 * experts_all))
    widened = moe_input.astype(jnp.float32)
    normal_in = (
        widened * lax.rsqrt(jnp.mean(widened * widened, axis=-1, keepdims=True) + 1e-06) * moe_gain
    ).astype(jnp.bfloat16)
    chosen = route_experts.reshape(-1)
    onehot = (chosen[:, None] == jnp.arange(experts_all, dtype=jnp.int32)[None, :]).astype(
        jnp.int32
    )
    slot_rank = jnp.sum(jnp.cumsum(onehot, axis=0) * onehot, axis=-1) - 1
    slot_index = jnp.where(
        slot_rank < capacity, chosen * capacity + slot_rank, experts_all * capacity
    )
    source_row = jnp.arange(rows * TOP, dtype=jnp.int32) // TOP
    slot_token = (
        jnp.full((experts_all * capacity,), rows, jnp.int32)
        .at[slot_index]
        .set(source_row, mode="drop")
    )
    padded_in = jnp.concatenate([normal_in, jnp.zeros((1, model_width), jnp.bfloat16)], 0)
    send_buffer = padded_in[slot_token].reshape(experts_all, capacity, model_width)
    arrived = lax.all_to_all(send_buffer, "ep", split_axis=0, concat_axis=0, tiled=True)
    flat_rows = arrived.reshape(-1, model_width)
    gate_act = jnp.dot(flat_rows, expert_gate[0], preferred_element_type=jnp.float32)
    up_act = jnp.dot(flat_rows, expert_up[0], preferred_element_type=jnp.float32)
    inner = (jax.nn.silu(gate_act) * up_act).astype(jnp.bfloat16)
    result = jnp.dot(inner, expert_down[0], preferred_element_type=jnp.float32).astype(jnp.bfloat16)
    returned = lax.all_to_all(
        result.reshape(arrived.shape), "ep", split_axis=0, concat_axis=0, tiled=True
    )
    returned_flat = jnp.concatenate(
        [
            returned.reshape(experts_all * capacity, model_width),
            jnp.zeros((1, model_width), jnp.bfloat16),
        ],
        0,
    )
    picked = returned_flat[slot_index].reshape(rows, TOP, model_width)
    group_gate = jax.nn.sigmoid(route_scores[:, 0])
    first_weight = (group_gate * jax.nn.sigmoid(route_scores[:, 1]))[:, None]
    second_weight = (group_gate * jax.nn.sigmoid(-route_scores[:, 1]))[:, None]
    combined = first_weight * picked[:, 0].astype(jnp.float32) + second_weight * picked[
        :, 1
    ].astype(jnp.float32)
    return combined.astype(jnp.bfloat16)


def swapped(x, axis, mask):
    peers = lax.axis_size(axis)
    return lax.ppermute(x, axis, [(i, i ^ mask) for i in range(peers)])


def partner_weights(expert_gate, expert_up, expert_down):
    peers = lax.axis_size("tp")
    share = expert_down.shape[1] // peers
    first = lax.axis_index("tp") * share
    gate_up = jnp.concatenate(
        [
            lax.dynamic_slice_in_dim(expert_gate[0], first, share, 1),
            lax.dynamic_slice_in_dim(expert_up[0], first, share, 1),
        ],
        1,
    )
    down = lax.dynamic_slice_in_dim(expert_down[0], first, share, 0)
    gate_ups = [swapped(gate_up, "ep", 1)]
    downs = [swapped(down, "ep", 1)]
    mask = peers // 2
    while mask:
        gate_ups = gate_ups + [swapped(piece, "tp", mask) for piece in gate_ups]
        downs = downs + [swapped(piece, "tp", mask) for piece in downs]
        mask //= 2
    gate = jnp.concatenate([piece[:, :share] for piece in gate_ups], 1)
    up = jnp.concatenate([piece[:, share:] for piece in gate_ups], 1)
    return gate, up, jnp.concatenate(downs, 0)


def one_expert(rows, gate, up, down):
    gate_act = jnp.dot(rows, gate, preferred_element_type=jnp.float32)
    up_act = jnp.dot(rows, up, preferred_element_type=jnp.float32)
    inner = (jax.nn.silu(gate_act) * up_act).astype(jnp.bfloat16)
    return jnp.dot(inner, down, preferred_element_type=jnp.float32).astype(jnp.bfloat16)


def pair_half(moe_input, moe_gain, route_experts, route_scores, expert_gate, expert_up, expert_down, first):
    rows, model_width = moe_input.shape
    experts_all = lax.axis_size("ep")
    groups = experts_all // TOP
    capacity = 2 * (3 * TOP * rows // (4 * experts_all))
    other = partner_weights(expert_gate, expert_up, expert_down)
    widened = moe_input.astype(jnp.float32)
    normal_in = (
        widened * lax.rsqrt(jnp.mean(widened * widened, axis=-1, keepdims=True) + 1e-06) * moe_gain
    ).astype(jnp.bfloat16)
    row_group = route_experts[:, 0] // TOP
    onehot = (row_group[:, None] == jnp.arange(groups, dtype=jnp.int32)[None, :]).astype(
        jnp.bfloat16
    )
    order = jnp.arange(rows, dtype=jnp.int32)
    before = (order[:, None] > order[None, :]).astype(jnp.bfloat16)
    ranks = jnp.dot(before, onehot, preferred_element_type=jnp.float32)
    rank = jnp.sum(ranks * onehot.astype(jnp.float32), axis=1).astype(jnp.int32)
    slot = jnp.where(rank < capacity, row_group * capacity + rank, -1)
    slots = jnp.arange(groups * capacity, dtype=jnp.int32)
    pick = (slots[:, None] == slot[None, :]).astype(jnp.bfloat16)
    group_gate = jax.nn.sigmoid(route_scores[:, 0])
    first_weight = group_gate * jax.nn.sigmoid(route_scores[:, 1])
    second_weight = group_gate * jax.nn.sigmoid(-route_scores[:, 1])
    in_order = route_experts[:, 0] % TOP == 0
    low_weight = jnp.where(in_order, first_weight, second_weight)
    high_weight = jnp.where(in_order, second_weight, first_weight)
    lane = jnp.arange(128, dtype=jnp.int32)[None, :]
    weights = jnp.where(lane < 64, low_weight[:, None], high_weight[:, None])
    coarse = lax.reduce_precision(weights, 8, 7)
    extra = jnp.where(lane % 64 < 32, coarse, weights - coarse).astype(jnp.bfloat16)
    sent = jnp.dot(
        pick, jnp.concatenate([normal_in, extra], 1), preferred_element_type=jnp.float32
    ).astype(jnp.bfloat16)
    sent, _ = lax.optimization_barrier((sent, first))
    along = [[TOP * g + x for g in range(groups)] for x in range(TOP)]
    arrived = lax.all_to_all(
        sent.reshape(groups, capacity, -1),
        "ep",
        split_axis=0,
        concat_axis=0,
        axis_index_groups=along,
        tiled=True,
    ).reshape(groups * capacity, -1)
    flat_rows = arrived[:, :model_width]
    tail = arrived[:, model_width:].astype(jnp.float32)
    low = tail[:, 0:1] + tail[:, 32:33]
    high = tail[:, 64:65] + tail[:, 96:97]
    even = lax.axis_index("ep") % TOP == 0
    mine = one_expert(flat_rows, expert_gate[0], expert_up[0], expert_down[0])
    theirs = one_expert(flat_rows, *other)
    combined = jnp.where(even, low, high) * mine.astype(jnp.float32) + jnp.where(
        even, high, low
    ) * theirs.astype(jnp.float32)
    returned = lax.all_to_all(
        combined.astype(jnp.bfloat16).reshape(groups, capacity, model_width),
        "ep",
        split_axis=0,
        concat_axis=0,
        axis_index_groups=along,
        tiled=True,
    ).reshape(groups * capacity, model_width)
    put = (slot[:, None] == slots[None, :]).astype(jnp.bfloat16)
    return jnp.dot(put, returned, preferred_element_type=jnp.float32).astype(jnp.bfloat16)


def on_device(
    conv_value,
    conv_gate,
    depth_weight,
    norm_gain,
    norm_shift,
    conv_out_weight,
    moe_input,
    moe_gain,
    route_experts,
    route_scores,
    expert_gate,
    expert_up,
    expert_down,
):
    gated, earlier = gate_and_halo(conv_value, conv_gate, depth_weight.shape[0] - 1)
    conv_out = conv_half(
        conv_value, gated, earlier, depth_weight, norm_gain, norm_shift, conv_out_weight
    )
    moe_args = (
        moe_input, moe_gain, route_experts, route_scores, expert_gate, expert_up, expert_down
    )
    if lax.axis_size("ep") // GROUPS == TOP:
        moe_out = pair_half(*moe_args, earlier)
    else:
        moe_out = moe_half(*moe_args)
    return (conv_out, moe_out)


def solution(mesh):
    in_specs = (
        P("ep", "tp"),
        P("ep", "tp"),
        P(),
        P(),
        P(),
        P("tp", None),
        P(("ep", "tp"), None),
        P(),
        P(("ep", "tp"), None),
        P(("ep", "tp"), None),
        P("ep", None, None),
        P("ep", None, None),
        P("ep", None, None),
    )
    out_specs = (P(("ep", "tp"), None), P(("ep", "tp"), None))
    return jax.shard_map(
        on_device, mesh=mesh, in_specs=in_specs, out_specs=out_specs, check_vma=False
    )
```

```python
import jax
import jax.numpy as jnp
from jax import lax
from jax.sharding import PartitionSpec as P

GROUPS = 4
TOP = 2


def passed_along(x, axis, by):
    peers = lax.axis_size(axis)
    pairs = [(i, i + by) for i in range(peers) if 0 <= i + by < peers]
    return lax.ppermute(x, axis, pairs)


def gated_rows(value, gate):
    return (value.astype(jnp.float32) * jax.nn.sigmoid(gate.astype(jnp.float32))).astype(
        jnp.bfloat16
    )


def conv_half(conv_value, conv_gate, earlier, depth_weight, norm_gain, norm_shift, conv_out_weight):
    channels = conv_value.shape[1]
    length = conv_value.shape[0]
    first_col = lax.axis_index("tp") * channels
    taps = lax.dynamic_slice_in_dim(depth_weight, first_col, channels, 1)
    gains = lax.dynamic_slice_in_dim(norm_gain, first_col, channels, 0)
    shifts = lax.dynamic_slice_in_dim(norm_shift, first_col, channels, 0)
    reach = taps.shape[0] - 1
    gated = gated_rows(conv_value, conv_gate)
    padded = jnp.concatenate([earlier, gated], 0).astype(jnp.float32)
    filtered = taps[0] * padded[0:length]
    for offset in range(1, reach + 1):
        filtered = filtered + taps[offset] * padded[offset : offset + length]
    sums, squares = lax.psum(
        (jnp.sum(filtered, axis=1), jnp.sum(filtered * filtered, axis=1)), "tp"
    )
    all_channels = channels * lax.axis_size("tp")
    center = (sums / all_channels)[:, None]
    spread = (squares / all_channels)[:, None] - center * center
    normed = (filtered - center) * lax.rsqrt(spread + 1e-05) * gains + shifts
    activated = jax.nn.silu(normed).astype(jnp.bfloat16)
    partial_value = jnp.dot(activated, conv_out_weight, preferred_element_type=jnp.float32)
    return partial_value.astype(jnp.bfloat16)


def scattered_sum(partial):
    peers = lax.axis_size("tp")
    me = lax.axis_index("tp")
    size = partial.shape[0] // peers
    total = lax.dynamic_slice_in_dim(partial, me * size, size, 0).astype(jnp.float32)
    for mask in range(peers - 1, 0, -1):
        block = lax.dynamic_slice_in_dim(partial, (me ^ mask) * size, size, 0)
        total = total + swapped(block, "tp", mask).astype(jnp.float32)
    return total.astype(jnp.bfloat16)


def moe_half(moe_input, moe_gain, route_experts, route_scores, expert_gate, expert_up, expert_down):
    rows = moe_input.shape[0]
    model_width = moe_input.shape[1]
    experts_all = lax.axis_size("ep")
    capacity = 2 * (3 * TOP * rows // (4 * experts_all))
    widened = moe_input.astype(jnp.float32)
    normal_in = (
        widened * lax.rsqrt(jnp.mean(widened * widened, axis=-1, keepdims=True) + 1e-06) * moe_gain
    ).astype(jnp.bfloat16)
    chosen = route_experts.reshape(-1)
    onehot = (chosen[:, None] == jnp.arange(experts_all, dtype=jnp.int32)[None, :]).astype(
        jnp.int32
    )
    slot_rank = jnp.sum(jnp.cumsum(onehot, axis=0) * onehot, axis=-1) - 1
    slot_index = jnp.where(
        slot_rank < capacity, chosen * capacity + slot_rank, experts_all * capacity
    )
    source_row = jnp.arange(rows * TOP, dtype=jnp.int32) // TOP
    slot_token = (
        jnp.full((experts_all * capacity,), rows, jnp.int32)
        .at[slot_index]
        .set(source_row, mode="drop")
    )
    padded_in = jnp.concatenate([normal_in, jnp.zeros((1, model_width), jnp.bfloat16)], 0)
    send_buffer = padded_in[slot_token].reshape(experts_all, capacity, model_width)
    arrived = lax.all_to_all(send_buffer, "ep", split_axis=0, concat_axis=0, tiled=True)
    flat_rows = arrived.reshape(-1, model_width)
    gate_act = jnp.dot(flat_rows, expert_gate[0], preferred_element_type=jnp.float32)
    up_act = jnp.dot(flat_rows, expert_up[0], preferred_element_type=jnp.float32)
    inner = (jax.nn.silu(gate_act) * up_act).astype(jnp.bfloat16)
    result = jnp.dot(inner, expert_down[0], preferred_element_type=jnp.float32).astype(jnp.bfloat16)
    returned = lax.all_to_all(
        result.reshape(arrived.shape), "ep", split_axis=0, concat_axis=0, tiled=True
    )
    returned_flat = jnp.concatenate(
        [
            returned.reshape(experts_all * capacity, model_width),
            jnp.zeros((1, model_width), jnp.bfloat16),
        ],
        0,
    )
    picked = returned_flat[slot_index].reshape(rows, TOP, model_width)
    group_gate = jax.nn.sigmoid(route_scores[:, 0])
    first_weight = (group_gate * jax.nn.sigmoid(route_scores[:, 1]))[:, None]
    second_weight = (group_gate * jax.nn.sigmoid(-route_scores[:, 1]))[:, None]
    combined = first_weight * picked[:, 0].astype(jnp.float32) + second_weight * picked[
        :, 1
    ].astype(jnp.float32)
    return combined.astype(jnp.bfloat16)


def swapped(x, axis, mask):
    peers = lax.axis_size(axis)
    return lax.ppermute(x, axis, [(i, i ^ mask) for i in range(peers)])


def partner_weights(expert_gate, expert_up, expert_down, place):
    peers = lax.axis_size("tp")
    share = expert_down.shape[1] // peers
    first = place * share
    gate_up = jnp.concatenate(
        [
            lax.dynamic_slice_in_dim(expert_gate[0], first, share, 1),
            lax.dynamic_slice_in_dim(expert_up[0], first, share, 1),
        ],
        1,
    )
    down = lax.dynamic_slice_in_dim(expert_down[0], first, share, 0)
    gate_ups = [swapped(gate_up, "ep", 1)]
    downs = [swapped(down, "ep", 1)]
    mask = peers // 2
    while mask:
        gate_ups = gate_ups + [swapped(piece, "tp", mask) for piece in gate_ups]
        downs = downs + [swapped(piece, "tp", mask) for piece in downs]
        mask //= 2
    gate = jnp.concatenate([piece[:, :share] for piece in gate_ups], 1)
    up = jnp.concatenate([piece[:, share:] for piece in gate_ups], 1)
    return gate, up, jnp.concatenate(downs, 0)


def one_expert(rows, gate, up, down):
    gate_act = jnp.dot(rows, gate, preferred_element_type=jnp.float32)
    up_act = jnp.dot(rows, up, preferred_element_type=jnp.float32)
    inner = (jax.nn.silu(gate_act) * up_act).astype(jnp.bfloat16)
    return jnp.dot(inner, down, preferred_element_type=jnp.float32).astype(jnp.bfloat16)


def pair_half(moe_input, moe_gain, route_experts, route_scores, expert_gate, expert_up, expert_down, first, beside):
    rows, model_width = moe_input.shape
    experts_all = lax.axis_size("ep")
    groups = experts_all // TOP
    capacity = 2 * (3 * TOP * rows // (4 * experts_all))
    widened = moe_input.astype(jnp.float32)
    normal_in = (
        widened * lax.rsqrt(jnp.mean(widened * widened, axis=-1, keepdims=True) + 1e-06) * moe_gain
    ).astype(jnp.bfloat16)
    row_group = route_experts[:, 0] // TOP
    onehot = (row_group[:, None] == jnp.arange(groups, dtype=jnp.int32)[None, :]).astype(
        jnp.bfloat16
    )
    order = jnp.arange(rows, dtype=jnp.int32)
    before = (order[:, None] > order[None, :]).astype(jnp.bfloat16)
    ranks = jnp.dot(before, onehot, preferred_element_type=jnp.float32)
    rank = jnp.sum(ranks * onehot.astype(jnp.float32), axis=1).astype(jnp.int32)
    slot = jnp.where(rank < capacity, row_group * capacity + rank, -1)
    slots = jnp.arange(groups * capacity, dtype=jnp.int32)
    pick = (slots[:, None] == slot[None, :]).astype(jnp.bfloat16)
    group_gate = jax.nn.sigmoid(route_scores[:, 0])
    first_weight = group_gate * jax.nn.sigmoid(route_scores[:, 1])
    second_weight = group_gate * jax.nn.sigmoid(-route_scores[:, 1])
    in_order = route_experts[:, 0] % TOP == 0
    low_weight = jnp.where(in_order, first_weight, second_weight)
    high_weight = jnp.where(in_order, second_weight, first_weight)
    lane = jnp.arange(128, dtype=jnp.int32)[None, :]
    weights = jnp.where(lane < 64, low_weight[:, None], high_weight[:, None])
    coarse = lax.reduce_precision(weights, 8, 7)
    extra = jnp.where(lane % 64 < 32, coarse, weights - coarse).astype(jnp.bfloat16)
    sent = jnp.dot(
        pick, jnp.concatenate([normal_in, extra], 1), preferred_element_type=jnp.float32
    ).astype(jnp.bfloat16)
    sent, _, place = lax.optimization_barrier((sent, first, lax.axis_index("tp")))
    other = partner_weights(expert_gate, expert_up, expert_down, place)
    along = [[TOP * g + x for g in range(groups)] for x in range(TOP)]
    arrived = lax.all_to_all(
        sent.reshape(groups, capacity, -1),
        "ep",
        split_axis=0,
        concat_axis=0,
        axis_index_groups=along,
        tiled=True,
    ).reshape(groups * capacity, -1)
    arrived, beside = lax.optimization_barrier((arrived, beside))
    flat_rows = arrived[:, :model_width]
    tail = arrived[:, model_width:].astype(jnp.float32)
    low = tail[:, 0:1] + tail[:, 32:33]
    high = tail[:, 64:65] + tail[:, 96:97]
    even = lax.axis_index("ep") % TOP == 0
    mine = one_expert(flat_rows, expert_gate[0], expert_up[0], expert_down[0])
    theirs = one_expert(flat_rows, *other)
    combined = jnp.where(even, low, high) * mine.astype(jnp.float32) + jnp.where(
        even, high, low
    ) * theirs.astype(jnp.float32)
    returned = lax.all_to_all(
        combined.astype(jnp.bfloat16).reshape(groups, capacity, model_width),
        "ep",
        split_axis=0,
        concat_axis=0,
        axis_index_groups=along,
        tiled=True,
    ).reshape(groups * capacity, model_width)
    put = (slot[:, None] == slots[None, :]).astype(jnp.bfloat16)
    moe_out = jnp.dot(put, returned, preferred_element_type=jnp.float32).astype(jnp.bfloat16)
    return moe_out, beside


def on_device(
    conv_value,
    conv_gate,
    depth_weight,
    norm_gain,
    norm_shift,
    conv_out_weight,
    moe_input,
    moe_gain,
    route_experts,
    route_scores,
    expert_gate,
    expert_up,
    expert_down,
):
    last = conv_value.shape[0] - depth_weight.shape[0] + 1
    earlier = passed_along(gated_rows(conv_value[last:], conv_gate[last:]), "ep", 1)
    partial = conv_half(
        conv_value, conv_gate, earlier, depth_weight, norm_gain, norm_shift, conv_out_weight
    )
    moe_args = (
        moe_input, moe_gain, route_experts, route_scores, expert_gate, expert_up, expert_down
    )
    if lax.axis_size("ep") // GROUPS == TOP:
        moe_out, partial = pair_half(*moe_args, earlier, partial)
    else:
        moe_out = moe_half(*moe_args)
    return (scattered_sum(partial), moe_out)


def solution(mesh):
    in_specs = (
        P("ep", "tp"),
        P("ep", "tp"),
        P(),
        P(),
        P(),
        P("tp", None),
        P(("ep", "tp"), None),
        P(),
        P(("ep", "tp"), None),
        P(("ep", "tp"), None),
        P("ep", None, None),
        P("ep", None, None),
        P("ep", None, None),
    )
    out_specs = (P(("ep", "tp"), None), P(("ep", "tp"), None))
    return jax.shard_map(
        on_device, mesh=mesh, in_specs=in_specs, out_specs=out_specs, check_vma=False
    )
```
